32 devices in a mesh: sp: 8 (over z, core), tp: 4 (over y, x).
Axes of the slice: x: 2, y: 2, z: 4, core: 2. Of those that a mesh axis runs over, the one named last changes fastest.
Arguments:
- prompt: bfloat16 [8, 2048, 2048], P('tp', 'sp'), may hold values from -6 to 6
- input_gain: float32 [2048], replicated, may hold values from 0.1 to 1.9
- key_weight: bfloat16 [1024, 2048], P('tp'), may hold values from -0.125 to 0.125
- value_weight: bfloat16 [1024, 2048], P('tp'), may hold values from -0.125 to 0.125
- key_gain: float32 [64], replicated, may hold values from 0.1 to 1.9
- queries: bfloat16 [8, 2, 1024], P('sp', None, 'tp'), may hold values from -6 to 6
- score_bias: float32 [2, 16], replicated, may hold values from -9 to -2
Outputs:
- keys: bfloat16 [8, 1024, 2048], P('sp', 'tp')
- values: bfloat16 [8, 1024, 2048], P('sp', 'tp')
- first_read: bfloat16 [8, 2, 1024], P('sp', None, 'tp')
The draws below stay inside these ranges and needn't reach their ends.
All inputs are finite; a program needn't handle non-finite values.
Results may differ from the reference program's by a relative error of at most 0.01.
Values may be sent and summed in bfloat16 or wider, within the bound.
A program may use at most 64 MiB of HBM per device.

```python
import math
import jax
import jax.numpy as jnp
from jax import lax

D = 2048
KV_HEADS = 16
HEAD = 64
GROUP = 2
SEQS = 8
LEN = 2048
KVW = 1024


def shard_levels(key, extent, split, low, high):
    def one(position, blocks):
        draws = jax.random.uniform(jax.random.fold_in(jax.random.fold_in(key, 6), position), (blocks,), jnp.float32, low / len(split), high / len(split))
        return jnp.repeat(jnp.exp(draws), extent[position] // blocks).reshape((-1,) + (1,) * (len(extent) - position - 1))

    loudness = one(*split[0])
    for cut in split[1:]:
        loudness = loudness * one(*cut)
    return loudness


def gaussian(stream_key, dims, scale, reach, shards=(), held_as=jnp.bfloat16):
    array = jax.random.normal(stream_key, dims, jnp.float32) * scale
    if len(shards) > 0:
        array = shard_levels(stream_key, dims, shards, -0.22, 0.18) * array
    return jnp.clip(array, min=-reach, max=reach).astype(held_as)


def setup_inputs(seed: int = 0) -> dict:
    key_of = jax.random.split(jax.random.key(seed), 8)
    prompt = gaussian(key_of[0], (SEQS, LEN, D), 1.0, 6.0, ((0, 4), (1, 8)))
    input_gain = jnp.clip(1.0 + 0.18 * jax.random.normal(key_of[1], (D,), jnp.float32), 0.1, 1.9)
    key_weight = gaussian(key_of[2], (KVW, D), D ** -0.5, 0.125, ((0, 4),))
    value_weight = gaussian(key_of[3], (KVW, D), D ** -0.5, 0.125, ((0, 4),))
    key_gain = jnp.clip(1.0 + 0.18 * jax.random.normal(key_of[4], (HEAD,), jnp.float32), 0.1, 1.9)
    queries = gaussian(key_of[5], (SEQS, GROUP, KVW), 1.0, 6.0, ((0, 8), (2, 4)))
    score_bias = jnp.clip(jax.random.uniform(key_of[6], (GROUP, KV_HEADS), jnp.float32, -9.0, -2.0), -9.0, -2.0)
    return dict(prompt=prompt, input_gain=input_gain, key_weight=key_weight, value_weight=value_weight, key_gain=key_gain, queries=queries, score_bias=score_bias)


epsilon = 1e-06

def reference(prompt, input_gain, key_weight, value_weight, key_gain, queries, score_bias):

    def one_sequence(pair):
        rows, query = pair
        flat = rows.astype(jnp.float32)
        normed = (flat * lax.rsqrt(lax.optimization_barrier(jnp.mean(flat * flat, axis=-1, keepdims=True)) + epsilon) * input_gain).astype(jnp.bfloat16)
        key_raw = jnp.dot(normed, key_weight.T, preferred_element_type=jnp.float32).reshape(LEN, KV_HEADS, HEAD)
        key_norm = (key_raw * lax.rsqrt(lax.optimization_barrier(jnp.mean(key_raw * key_raw, axis=-1, keepdims=True)) + epsilon) * key_gain).astype(jnp.bfloat16)
        value_rows = jnp.dot(normed, value_weight.T, preferred_element_type=jnp.float32).astype(jnp.bfloat16)
        query_heads = query.astype(jnp.float32).reshape(GROUP, KV_HEADS, HEAD)
        scores = jnp.einsum('ghd,shd->ghs', query_heads, key_norm.astype(jnp.float32)) / math.sqrt(HEAD)
        scores = scores + score_bias[:, :, None]
        log_break = jax.nn.log_sigmoid(scores)
        log_keep = jax.nn.log_sigmoid(-scores)
        later = lax.cumsum(log_keep, axis=2, reverse=True) - log_keep
        weights = jnp.exp(log_break + later).astype(jnp.bfloat16)
        value_heads = value_rows.astype(jnp.float32).reshape(LEN, KV_HEADS, HEAD)
        read = jnp.einsum('ghs,shd->ghd', weights.astype(jnp.float32), value_heads).astype(jnp.bfloat16)
        return (key_norm.reshape(LEN, KVW).T, value_rows.T, read.reshape(GROUP, KVW))
    keys, values, first_read = lax.map(one_sequence, (prompt, queries))
    return (keys, values, first_read)
```

```python
import functools
import math

import jax
import jax.numpy as jnp
from jax import lax
from jax.experimental import pallas as pl
from jax.experimental.pallas import tpu as pltpu
from jax.sharding import PartitionSpec as P

HEAD = 64
LANES = 128
CORES = 2
NORM_ROWS = 16
W_CHUNKS = 4

epsilon = 1e-06
MESH = pl.DeviceIdType.MESH


def produce(
    dims, prompt, gain, key_w, value_w, key_gain, cache,
    x, xn, w, out, relay, gain_column,
    x_in, w_in, x_send, x_recv, w_send, w_recv, f_send, f_recv, h_send, h_recv, o_send, o_recv,
):
    sp, tp, A, B, R, halves, cols, width = dims
    s, t = lax.axis_index("sp"), lax.axis_index("tp")
    yb, xa = t // A, t % A
    core = s % CORES
    partner = s + 1 - 2 * core
    seqs = R // halves
    w_rows = cols // W_CHUNKS

    def local_x(i):
        return pltpu.make_async_copy(prompt.at[i], x.at[i], x_in.at[i])

    def local_w(k):
        return pltpu.make_async_copy((key_w, value_w)[k], w.at[0, k], w_in.at[k])

    for k in range(2):
        local_w(k).start()
    for i in range(R):
        local_x(i).start()

    def row_peer(db):
        return ((yb + db) % B) * A + xa

    def column_peer(da):
        return yb * A + (xa + da) % A

    barrier = pltpu.get_barrier_semaphore()

    def greet(k, _):
        other = lax.rem(s + k, sp)
        pl.semaphore_signal(barrier, inc=1, device_id={"sp": other, "tp": t}, device_id_type=MESH)
        return 0

    lax.fori_loop(1, sp, greet, 0)
    for da in range(1, A):
        pl.semaphore_signal(barrier, inc=1, device_id={"sp": s, "tp": column_peer(da)}, device_id_type=MESH)
    for db in range(1, B):
        pl.semaphore_signal(barrier, inc=1, device_id={"sp": s, "tp": row_peer(db)}, device_id_type=MESH)
    pl.semaphore_wait(barrier, sp - 1 + A - 1 + B - 1)

    def send_w(da, k):
        rows = pl.ds(k * w_rows, w_rows)
        return pltpu.make_async_remote_copy(
            src_ref=w.at[0, core, rows], dst_ref=w.at[da, core, rows],
            send_sem=w_send.at[da - 1, k], recv_sem=w_recv.at[da - 1, k],
            device_id={"sp": s, "tp": column_peer(da)}, device_id_type=MESH,
        )

    def forward_w(da, k):
        rows = pl.ds(k * w_rows, w_rows)
        return pltpu.make_async_remote_copy(
            src_ref=w.at[da, core, rows], dst_ref=w.at[da, core, rows],
            send_sem=f_send.at[da - 1, k], recv_sem=f_recv.at[da - 1, k],
            device_id={"sp": partner, "tp": t}, device_id_type=MESH,
        )

    def arrived_w(da, k):
        rows = pl.ds(k * w_rows, w_rows)
        return pltpu.make_async_remote_copy(
            src_ref=w.at[da, 1 - core, rows], dst_ref=w.at[da, 1 - core, rows],
            send_sem=f_send.at[da - 1, k], recv_sem=f_recv.at[da - 1, k],
            device_id={"sp": partner, "tp": t}, device_id_type=MESH,
        )

    def send_x(db, i):
        return pltpu.make_async_remote_copy(
            src_ref=x.at[i], dst_ref=x.at[db * R + i],
            send_sem=x_send.at[(db - 1) * R + i], recv_sem=x_recv.at[(db - 1) * R + i],
            device_id={"sp": s, "tp": row_peer(db)}, device_id_type=MESH,
        )

    for k in range(2):
        local_w(k).wait()
    for k in range(W_CHUNKS):
        for da in range(1, A):
            send_w(da, k).start()
    for i in range(R):
        local_x(i).wait()
        for db in range(1, B):
            send_x(db, i).start()

    def normalise(r):
        for k in range(LANES // NORM_ROWS):
            here = pl.ds(k * NORM_ROWS, NORM_ROWS)
            flat = x[r, here, :].astype(jnp.float32)
            scale = lax.rsqrt(jnp.mean(flat * flat, axis=-1, keepdims=True) + epsilon)
            xn[r, here, :] = (flat * scale * gain[...]).astype(jnp.bfloat16)

    eye = lax.broadcasted_iota(jnp.int32, (HEAD, HEAD), 0) == lax.broadcasted_iota(jnp.int32, (HEAD, HEAD), 1)
    gain_column[...] = jnp.broadcast_to(
        jnp.sum(jnp.where(eye, key_gain[...], 0.0), axis=1, keepdims=True), (HEAD, LANES)
    )

    class Home:
        def __init__(self, r, da):
            db, i = r // R, r % R
            j, half = i // halves, i % halves
            rows_of = ((yb + B - db) % B) * A + (xa + da) % A
            seq = rows_of * seqs + j
            slot = r * A + da
            index = s * halves + half
            place = cache.at[:, :, pl.ds(pl.multiple_of(index * LANES, LANES), LANES)]
            block = out.at[r, 0] if isinstance(da, int) and da == 0 else relay.at[r, da - 1]
            self.here = seq == s
            self.remote = pltpu.make_async_remote_copy(
                src_ref=block, dst_ref=place, send_sem=o_send.at[slot], recv_sem=o_recv.at[index],
                device_id={"sp": seq, "tp": t}, device_id_type=MESH,
            )
            self.block, self.place, self.sem = block, place, o_recv.at[index]

        def start(self):
            @pl.when(self.here)
            def _():
                self.place[...] = self.block[...]

            @pl.when(jnp.logical_not(self.here))
            def _():
                self.remote.start()

        def wait_send(self):
            @pl.when(jnp.logical_not(self.here))
            def _():
                self.remote.wait_send()

    def hop(r, da):
        return pltpu.make_async_remote_copy(
            src_ref=out.at[r, da], dst_ref=relay.at[r, da - 1],
            send_sem=h_send.at[r, da - 1], recv_sem=h_recv.at[r, da - 1],
            device_id={"sp": s, "tp": yb * A + (xa + A - da) % A}, device_id_type=MESH,
        )

    def project(r, da):
        rows = xn[r]
        contract = (((1,), (1,)), ((), ()))
        raw = lax.dot_general(w[da, 0], rows, contract, preferred_element_type=jnp.float32)
        raw = raw.reshape(cols // HEAD, HEAD, LANES)
        scale = lax.rsqrt(jnp.mean(raw * raw, axis=1, keepdims=True) + epsilon)
        keys = raw * scale * gain_column[...][None]
        out[r, da, 0] = keys.reshape(cols, LANES).astype(jnp.bfloat16)
        out[r, da, 1] = lax.dot_general(
            w[da, 1], rows, contract, preferred_element_type=jnp.float32
        ).astype(jnp.bfloat16)

    def keep(r):
        project(r, 0)
        Home(r, 0).start()

    def give(r):
        def one(da, _):
            project(r, da)
            hop(r, da).start()
            return 0

        lax.fori_loop(1, A, one, 0)

    def pass_on(r):
        for da in range(1, A):
            hop(r, da).wait_recv()
            Home(r, da).start()

    def own_first(r, _):
        normalise(r)
        keep(r)
        return 0

    lax.fori_loop(0, R, own_first, 0)

    def take(n):
        i, db = n // (B - 1), 1 + n % (B - 1)
        send_x(db, i).wait_recv()
        r = db * R + i
        normalise(r)
        keep(r)
        return r

    N = R * (B - 1)
    theirs = [(1 + n % (B - 1)) * R + n // (B - 1) for n in range(N)]
    early = N // 2
    taken = 0
    for k in range(W_CHUNKS):
        for da in range(1, A):
            send_w(da, k).wait_recv()
            forward_w(da, k).start()
        while taken < early * (k + 1) // W_CHUNKS:
            take(taken)
            taken += 1
    for k in range(W_CHUNKS):
        for da in range(1, A):
            arrived_w(da, k).wait_recv()

    order = []
    for n in range(max(early, R)):
        order += theirs[n : n + 1] if n < early else []
        order += [n] if n < R else []
    order += theirs[early:]
    given, passed = 0, 0
    for r in order[: early + R]:
        give(r)
        given += 1
        if given > early:
            pass_on(order[passed])
            passed += 1
    for n in range(early, N):
        give(take(n))
        given += 1
        while passed < min(R + 2 * (n - early + 1), given if n == N - 1 else given - 1):
            pass_on(order[passed])
            passed += 1
    while passed < len(order):
        pass_on(order[passed])
        passed += 1

    for k in range(W_CHUNKS):
        for da in range(1, A):
            send_w(da, k).wait_send()
            forward_w(da, k).wait_send()
    for i in range(R):
        for db in range(1, B):
            send_x(db, i).wait_send()

    for r in range(B * R):
        for da in range(A):
            Home(r, da).wait_send()
            if da:
                hop(r, da).wait_send()

    def arrived(n):
        place = cache.at[:, :, pl.ds(pl.multiple_of(n * LANES, LANES), LANES)]
        pltpu.make_async_copy(out.at[0, 0], place, o_recv.at[n]).wait()

    def landed(n, _):
        @pl.when(n // halves != s)
        def _():
            arrived(n)

        return 0

    lax.fori_loop(0, sp * halves, landed, 0)


def read(dims, queries, bias, cache, keys_out, values_out, first_out, sems):
    group, heads, cols, length = dims
    rows = group * heads
    t = lax.axis_index("tp")
    keys, values = cache.at[0], cache.at[1]
    out_k = pltpu.make_async_copy(keys, keys_out.at[0], sems.at[2])
    out_v = pltpu.make_async_copy(values, values_out.at[0], sems.at[3])
    out_k.start()
    out_v.start()

    def spread(ref_value):
        n = ref_value.shape[1]
        parts = [jnp.broadcast_to(ref_value[g : g + 1], (heads, n)) for g in range(group)]
        return jnp.concatenate(parts, axis=0)

    row_head = lax.broadcasted_iota(jnp.int32, (rows, cols), 0) % heads
    own = (lax.broadcasted_iota(jnp.int32, (rows, cols), 1) // HEAD) == row_head
    query = jnp.where(own, spread(queries[...].astype(jnp.float32)), 0.0).astype(jnp.bfloat16)
    offsets = spread(bias[...])
    at = lax.broadcasted_iota(jnp.int32, offsets.shape, 1)
    mine = at == t * heads + lax.broadcasted_iota(jnp.int32, offsets.shape, 0) % heads
    offset = jnp.sum(jnp.where(mine, offsets, 0.0), axis=1, keepdims=True)

    scores = jnp.dot(query, keys[...], preferred_element_type=jnp.float32)
    scores = scores / math.sqrt(HEAD) + offset
    soft = jnp.log1p(jnp.exp(-jnp.abs(scores)))
    log_break = jnp.minimum(scores, 0.0) - soft
    log_keep = jnp.minimum(-scores, 0.0) - soft
    lane = lax.broadcasted_iota(jnp.int32, (rows, length), 1)

    def ahead(v, k):
        return jnp.where(lane < length - k, pltpu.roll(v, length - k, 1), 0.0)

    later = ahead(log_keep, 1)
    k = 1
    while k < length:
        later = later + ahead(later, k)
        k *= 2
    weights = jnp.exp(log_break + later).astype(jnp.bfloat16)
    taken = lax.dot_general(
        weights, values[...], (((1,), (1,)), ((), ())), preferred_element_type=jnp.float32
    )
    taken = jnp.where(own, taken, 0.0)
    for g in range(group):
        first_out[g : g + 1, :] = jnp.sum(
            taken[g * heads : (g + 1) * heads], axis=0, keepdims=True
        ).astype(jnp.bfloat16)
    out_k.wait()
    out_v.wait()


def local(prompt, input_gain, key_weight, value_weight, key_gain, queries, score_bias):
    sp, tp = lax.axis_size("sp"), lax.axis_size("tp")
    seq_here, pos_here, width = prompt.shape
    cols = key_weight.shape[0]
    group = queries.shape[1]
    A = 2 ** (int(math.log2(tp)) // 2)
    B = tp // A
    halves = pos_here // LANES
    R = seq_here * halves
    length = pos_here * sp
    hbm, vmem = pl.BlockSpec(memory_space=pl.ANY), pl.BlockSpec(memory_space=pltpu.VMEM)
    dma = pltpu.SemaphoreType.DMA
    bf16 = jnp.bfloat16
    cache = pl.pallas_call(
        functools.partial(produce, (sp, tp, A, B, R, halves, cols, width)),
        out_shape=pltpu.VMEM((2, cols, length), bf16),
        in_specs=[hbm, vmem, hbm, hbm, vmem],
        out_specs=vmem,
        scratch_shapes=[
            pltpu.VMEM((B * R, LANES, width), bf16),
            pltpu.VMEM((B * R, LANES, width), bf16),
            pltpu.VMEM((A, 2, cols, width), bf16),
            pltpu.VMEM((B * R, A, 2, cols, LANES), bf16),
            pltpu.VMEM((B * R, A - 1, 2, cols, LANES), bf16),
            pltpu.VMEM((HEAD, LANES), jnp.float32),
            dma((R,)),
            dma((2,)),
            dma(((B - 1) * R,)),
            dma(((B - 1) * R,)),
            dma((A - 1, W_CHUNKS)),
            dma((A - 1, W_CHUNKS)),
            dma((A - 1, W_CHUNKS)),
            dma((A - 1, W_CHUNKS)),
            dma((B * R, A - 1)),
            dma((B * R, A - 1)),
            dma((B * R * A,)),
            dma((sp * halves,)),
        ],
        compiler_params=pltpu.CompilerParams(
            collective_id=0, has_side_effects=True, vmem_limit_bytes=56 * 1024 * 1024
        ),
        name="produce",
    )(
        prompt.reshape(R, LANES, width),
        input_gain.reshape(1, width),
        key_weight,
        value_weight,
        key_gain.reshape(1, HEAD),
    )
    cache = pltpu.with_memory_space_constraint(cache, pltpu.VMEM)
    keys, values, first = pl.pallas_call(
        functools.partial(read, (group, cols // HEAD, cols, length)),
        out_shape=(
            jax.ShapeDtypeStruct((1, cols, length), bf16),
            jax.ShapeDtypeStruct((1, cols, length), bf16),
            jax.ShapeDtypeStruct((group, cols), bf16),
        ),
        in_specs=[vmem, vmem, vmem],
        out_specs=(hbm, hbm, vmem),
        scratch_shapes=[dma((4,))],
        name="read",
    )(queries.reshape(group, cols), score_bias, cache)
    return keys, values, first.reshape(1, group, cols)


def solution(mesh):
    placed = (P("tp", "sp", None), P(), P("tp", None), P("tp", None), P(), P("sp", None, "tp"), P())
    return jax.shard_map(
        local,
        mesh=mesh,
        in_specs=placed,
        out_specs=(P("sp", "tp", None), P("sp", "tp", None), P("sp", None, "tp")),
        check_vma=False,
    )
```

```python
import functools
import math

import jax
import jax.numpy as jnp
from jax import lax
from jax.experimental import pallas as pl
from jax.experimental.pallas import tpu as pltpu
from jax.sharding import PartitionSpec as P

HEAD = 64
LANES = 128
CORES = 2
NORM_ROWS = 16
W_CHUNKS = 4

epsilon = 1e-06
MESH = pl.DeviceIdType.MESH


def produce(
    dims, prompt, gain, key_w, value_w, key_gain, cache,
    x, xn, w, out, relay, gain_column,
    x_in, w_in, x_send, x_recv, w_send, w_recv, f_send, f_recv, h_send, h_recv, o_send, o_recv,
):
    sp, tp, A, B, R, halves, cols, width = dims
    s, t = lax.axis_index("sp"), lax.axis_index("tp")
    yb, xa = t // A, t % A
    core = s % CORES
    partner = s + 1 - 2 * core
    seqs = R // halves
    w_rows = cols // W_CHUNKS

    def local_x(i):
        return pltpu.make_async_copy(prompt.at[i], x.at[i], x_in.at[i])

    def local_w(k):
        return pltpu.make_async_copy((key_w, value_w)[k], w.at[0, k], w_in.at[k])

    for k in range(2):
        local_w(k).start()
    for i in range(R):
        local_x(i).start()

    def row_peer(db):
        return ((yb + db) % B) * A + xa

    def column_peer(da):
        return yb * A + (xa + da) % A

    barrier = pltpu.get_barrier_semaphore()

    def greet(k, _):
        other = lax.rem(s + k, sp)
        pl.semaphore_signal(barrier, inc=1, device_id={"sp": other, "tp": t}, device_id_type=MESH)
        return 0

    lax.fori_loop(1, sp, greet, 0)
    for da in range(1, A):
        pl.semaphore_signal(barrier, inc=1, device_id={"sp": s, "tp": column_peer(da)}, device_id_type=MESH)
    for db in range(1, B):
        pl.semaphore_signal(barrier, inc=1, device_id={"sp": s, "tp": row_peer(db)}, device_id_type=MESH)
    pl.semaphore_wait(barrier, sp - 1 + A - 1 + B - 1)

    def send_w(da, k):
        rows = pl.ds(k * w_rows, w_rows)
        return pltpu.make_async_remote_copy(
            src_ref=w.at[0, core, rows], dst_ref=w.at[da, core, rows],
            send_sem=w_send.at[da - 1, k], recv_sem=w_recv.at[da - 1, k],
            device_id={"sp": s, "tp": column_peer(da)}, device_id_type=MESH,
        )

    def forward_w(da, k):
        rows = pl.ds(k * w_rows, w_rows)
        return pltpu.make_async_remote_copy(
            src_ref=w.at[da, core, rows], dst_ref=w.at[da, core, rows],
            send_sem=f_send.at[da - 1, k], recv_sem=f_recv.at[da - 1, k],
            device_id={"sp": partner, "tp": t}, device_id_type=MESH,
        )

    def arrived_w(da, k):
        rows = pl.ds(k * w_rows, w_rows)
        return pltpu.make_async_remote_copy(
            src_ref=w.at[da, 1 - core, rows], dst_ref=w.at[da, 1 - core, rows],
            send_sem=f_send.at[da - 1, k], recv_sem=f_recv.at[da - 1, k],
            device_id={"sp": partner, "tp": t}, device_id_type=MESH,
        )

    def send_x(db, i):
        return pltpu.make_async_remote_copy(
            src_ref=x.at[i], dst_ref=x.at[db * R + i],
            send_sem=x_send.at[(db - 1) * R + i], recv_sem=x_recv.at[(db - 1) * R + i],
            device_id={"sp": s, "tp": row_peer(db)}, device_id_type=MESH,
        )

    for k in range(2):
        local_w(k).wait()
    for k in range(W_CHUNKS):
        for da in range(1, A):
            send_w(da, k).start()
    for i in range(R):
        local_x(i).wait()
        for db in range(1, B):
            send_x(db, i).start()

    def normalise(r):
        for k in range(LANES // NORM_ROWS):
            here = pl.ds(k * NORM_ROWS, NORM_ROWS)
            flat = x[r, here, :].astype(jnp.float32)
            scale = lax.rsqrt(jnp.mean(flat * flat, axis=-1, keepdims=True) + epsilon)
            xn[r, here, :] = (flat * scale * gain[...]).astype(jnp.bfloat16)

    eye = lax.broadcasted_iota(jnp.int32, (HEAD, HEAD), 0) == lax.broadcasted_iota(jnp.int32, (HEAD, HEAD), 1)
    gain_column[...] = jnp.broadcast_to(
        jnp.sum(jnp.where(eye, key_gain[...], 0.0), axis=1, keepdims=True), (HEAD, LANES)
    )

    class Home:
        def __init__(self, r, da):
            db, i = r // R, r % R
            j, half = i // halves, i % halves
            rows_of = ((yb + B - db) % B) * A + (xa + da) % A
            seq = rows_of * seqs + j
            slot = r * A + da
            index = s * halves + half
            place = cache.at[:, :, pl.ds(pl.multiple_of(index * LANES, LANES), LANES)]
            block = out.at[r, 0] if isinstance(da, int) and da == 0 else relay.at[r, da - 1]
            self.here = seq == s
            self.remote = pltpu.make_async_remote_copy(
                src_ref=block, dst_ref=place, send_sem=o_send.at[slot], recv_sem=o_recv.at[index],
                device_id={"sp": seq, "tp": t}, device_id_type=MESH,
            )
            self.block, self.place, self.sem = block, place, o_recv.at[index]

        def start(self):
            @pl.when(self.here)
            def _():
                self.place[...] = self.block[...]

            @pl.when(jnp.logical_not(self.here))
            def _():
                self.remote.start()

        def wait_send(self):
            @pl.when(jnp.logical_not(self.here))
            def _():
                self.remote.wait_send()

    def hop(r, da):
        return pltpu.make_async_remote_copy(
            src_ref=out.at[r, da], dst_ref=relay.at[r, da - 1],
            send_sem=h_send.at[r, da - 1], recv_sem=h_recv.at[r, da - 1],
            device_id={"sp": s, "tp": yb * A + (xa + A - da) % A}, device_id_type=MESH,
        )

    def project(r, da):
        rows = xn[r]
        contract = (((1,), (1,)), ((), ()))
        raw = lax.dot_general(w[da, 0], rows, contract, preferred_element_type=jnp.float32)
        raw = raw.reshape(cols // HEAD, HEAD, LANES)
        scale = lax.rsqrt(jnp.mean(raw * raw, axis=1, keepdims=True) + epsilon)
        keys = raw * scale * gain_column[...][None]
        out[r, da, 0] = keys.reshape(cols, LANES).astype(jnp.bfloat16)
        out[r, da, 1] = lax.dot_general(
            w[da, 1], rows, contract, preferred_element_type=jnp.float32
        ).astype(jnp.bfloat16)

    def keep(r):
        project(r, 0)
        Home(r, 0).start()

    def give(r):
        def one(da, _):
            project(r, da)
            hop(r, da).start()
            return 0

        lax.fori_loop(1, A, one, 0)

    def pass_on(r):
        for da in range(1, A):
            hop(r, da).wait_recv()
            Home(r, da).start()

    def own_first(r, _):
        normalise(r)
        keep(r)
        return 0

    lax.fori_loop(0, R, own_first, 0)

    def take(n):
        i, db = n // (B - 1), 1 + n % (B - 1)
        send_x(db, i).wait_recv()
        r = db * R + i
        normalise(r)
        keep(r)
        return r

    N = R * (B - 1)
    theirs = [(1 + n % (B - 1)) * R + n // (B - 1) for n in range(N)]
    early = N // 2
    taken = 0
    for k in range(W_CHUNKS):
        for da in range(1, A):
            send_w(da, k).wait_recv()
            forward_w(da, k).start()
        while taken < early * (k + 1) // W_CHUNKS:
            take(taken)
            taken += 1
    for k in range(W_CHUNKS):
        for da in range(1, A):
            arrived_w(da, k).wait_recv()

    stays = (2 * t * seqs >= sp) == (2 * s >= sp)
    others_first = theirs[:early] + list(range(R))
    own_first_order = list(range(R)) + theirs[:early]
    order = [jnp.where(stays, a, b) for a, b in zip(others_first, own_first_order)]
    order += theirs[early:]
    given, passed = 0, 0
    for r in order[: early + R]:
        give(r)
        given += 1
        if given > early:
            pass_on(order[passed])
            passed += 1
    for n in range(early, N):
        give(take(n))
        given += 1
        while passed < (given if n == N - 1 else given - 1):
            pass_on(order[passed])
            passed += 1
    while passed < len(order):
        pass_on(order[passed])
        passed += 1

    for k in range(W_CHUNKS):
        for da in range(1, A):
            send_w(da, k).wait_send()
            forward_w(da, k).wait_send()
    for i in range(R):
        for db in range(1, B):
            send_x(db, i).wait_send()

    for r in range(B * R):
        for da in range(A):
            Home(r, da).wait_send()
            if da:
                hop(r, da).wait_send()

    def arrived(n):
        place = cache.at[:, :, pl.ds(pl.multiple_of(n * LANES, LANES), LANES)]
        pltpu.make_async_copy(out.at[0, 0], place, o_recv.at[n]).wait()

    def landed(n, _):
        @pl.when(n // halves != s)
        def _():
            arrived(n)

        return 0

    lax.fori_loop(0, sp * halves, landed, 0)


def read(dims, queries, bias, cache, keys_out, values_out, first_out, sems):
    group, heads, cols, length = dims
    rows = group * heads
    t = lax.axis_index("tp")
    keys, values = cache.at[0], cache.at[1]
    out_k = pltpu.make_async_copy(keys, keys_out.at[0], sems.at[2])
    out_v = pltpu.make_async_copy(values, values_out.at[0], sems.at[3])
    out_k.start()
    out_v.start()

    def spread(ref_value):
        n = ref_value.shape[1]
        parts = [jnp.broadcast_to(ref_value[g : g + 1], (heads, n)) for g in range(group)]
        return jnp.concatenate(parts, axis=0)

    row_head = lax.broadcasted_iota(jnp.int32, (rows, cols), 0) % heads
    own = (lax.broadcasted_iota(jnp.int32, (rows, cols), 1) // HEAD) == row_head
    query = jnp.where(own, spread(queries[...].astype(jnp.float32)), 0.0).astype(jnp.bfloat16)
    offsets = spread(bias[...])
    at = lax.broadcasted_iota(jnp.int32, offsets.shape, 1)
    mine = at == t * heads + lax.broadcasted_iota(jnp.int32, offsets.shape, 0) % heads
    offset = jnp.sum(jnp.where(mine, offsets, 0.0), axis=1, keepdims=True)

    scores = jnp.dot(query, keys[...], preferred_element_type=jnp.float32)
    scores = scores / math.sqrt(HEAD) + offset
    soft = jnp.log1p(jnp.exp(-jnp.abs(scores)))
    log_break = jnp.minimum(scores, 0.0) - soft
    log_keep = jnp.minimum(-scores, 0.0) - soft
    lane = lax.broadcasted_iota(jnp.int32, (rows, length), 1)

    def ahead(v, k):
        return jnp.where(lane < length - k, pltpu.roll(v, length - k, 1), 0.0)

    later = ahead(log_keep, 1)
    k = 1
    while k < length:
        later = later + ahead(later, k)
        k *= 2
    weights = jnp.exp(log_break + later).astype(jnp.bfloat16)
    taken = lax.dot_general(
        weights, values[...], (((1,), (1,)), ((), ())), preferred_element_type=jnp.float32
    )
    taken = jnp.where(own, taken, 0.0)
    for g in range(group):
        first_out[g : g + 1, :] = jnp.sum(
            taken[g * heads : (g + 1) * heads], axis=0, keepdims=True
        ).astype(jnp.bfloat16)
    out_k.wait()
    out_v.wait()


def local(prompt, input_gain, key_weight, value_weight, key_gain, queries, score_bias):
    sp, tp = lax.axis_size("sp"), lax.axis_size("tp")
    seq_here, pos_here, width = prompt.shape
    cols = key_weight.shape[0]
    group = queries.shape[1]
    A = 2 ** (int(math.log2(tp)) // 2)
    B = tp // A
    halves = pos_here // LANES
    R = seq_here * halves
    length = pos_here * sp
    hbm, vmem = pl.BlockSpec(memory_space=pl.ANY), pl.BlockSpec(memory_space=pltpu.VMEM)
    dma = pltpu.SemaphoreType.DMA
    bf16 = jnp.bfloat16
    cache = pl.pallas_call(
        functools.partial(produce, (sp, tp, A, B, R, halves, cols, width)),
        out_shape=pltpu.VMEM((2, cols, length), bf16),
        in_specs=[hbm, vmem, hbm, hbm, vmem],
        out_specs=vmem,
        scratch_shapes=[
            pltpu.VMEM((B * R, LANES, width), bf16),
            pltpu.VMEM((B * R, LANES, width), bf16),
            pltpu.VMEM((A, 2, cols, width), bf16),
            pltpu.VMEM((B * R, A, 2, cols, LANES), bf16),
            pltpu.VMEM((B * R, A - 1, 2, cols, LANES), bf16),
            pltpu.VMEM((HEAD, LANES), jnp.float32),
            dma((R,)),
            dma((2,)),
            dma(((B - 1) * R,)),
            dma(((B - 1) * R,)),
            dma((A - 1, W_CHUNKS)),
            dma((A - 1, W_CHUNKS)),
            dma((A - 1, W_CHUNKS)),
            dma((A - 1, W_CHUNKS)),
            dma((B * R, A - 1)),
            dma((B * R, A - 1)),
            dma((B * R * A,)),
            dma((sp * halves,)),
        ],
        compiler_params=pltpu.CompilerParams(
            collective_id=0, has_side_effects=True, vmem_limit_bytes=56 * 1024 * 1024
        ),
        name="produce",
    )(
        prompt.reshape(R, LANES, width),
        input_gain.reshape(1, width),
        key_weight,
        value_weight,
        key_gain.reshape(1, HEAD),
    )
    cache = pltpu.with_memory_space_constraint(cache, pltpu.VMEM)
    keys, values, first = pl.pallas_call(
        functools.partial(read, (group, cols // HEAD, cols, length)),
        out_shape=(
            jax.ShapeDtypeStruct((1, cols, length), bf16),
            jax.ShapeDtypeStruct((1, cols, length), bf16),
            jax.ShapeDtypeStruct((group, cols), bf16),
        ),
        in_specs=[vmem, vmem, vmem],
        out_specs=(hbm, hbm, vmem),
        scratch_shapes=[dma((4,))],
        name="read",
    )(queries.reshape(group, cols), score_bias, cache)
    return keys, values, first.reshape(1, group, cols)


def solution(mesh):
    placed = (P("tp", "sp", None), P(), P("tp", None), P("tp", None), P(), P("sp", None, "tp"), P())
    return jax.shard_map(
        local,
        mesh=mesh,
        in_specs=placed,
        out_specs=(P("sp", "tp", None), P("sp", "tp", None), P("sp", None, "tp")),
        check_vma=False,
    )
```

```python
import functools
import math

import jax
import jax.numpy as jnp
from jax import lax
from jax.experimental import pallas as pl
from jax.experimental.pallas import tpu as pltpu
from jax.sharding import PartitionSpec as P

HEAD = 64
LANES = 128
CORES = 2
NORM_ROWS = 16
W_CHUNKS = 4

epsilon = 1e-06
MESH = pl.DeviceIdType.MESH


def produce(
    dims, prompt, gain, key_w, value_w, key_gain, cache,
    x, xn, w, out, relay, gain_column,
    x_in, w_in, x_send, x_recv, w_send, w_recv, f_send, f_recv, h_send, h_recv, o_send, o_recv,
):
    sp, tp, A, B, R, halves, cols, width = dims
    s, t = lax.axis_index("sp"), lax.axis_index("tp")
    yb, xa = t // A, t % A
    core = s % CORES
    partner = s + 1 - 2 * core
    seqs = R // halves
    w_rows = cols // W_CHUNKS

    def local_x(i):
        return pltpu.make_async_copy(prompt.at[i], x.at[i], x_in.at[i])

    def local_w(k):
        return pltpu.make_async_copy((key_w, value_w)[k], w.at[0, k], w_in.at[k])

    for k in range(2):
        local_w(k).start()
    for i in range(R):
        local_x(i).start()

    def row_peer(db):
        return ((yb + db) % B) * A + xa

    def column_peer(da):
        return yb * A + (xa + da) % A

    barrier = pltpu.get_barrier_semaphore()

    def greet(k, _):
        other = lax.rem(s + k, sp)
        pl.semaphore_signal(barrier, inc=1, device_id={"sp": other, "tp": t}, device_id_type=MESH)
        return 0

    lax.fori_loop(1, sp, greet, 0)
    for da in range(1, A):
        pl.semaphore_signal(barrier, inc=1, device_id={"sp": s, "tp": column_peer(da)}, device_id_type=MESH)
    for db in range(1, B):
        pl.semaphore_signal(barrier, inc=1, device_id={"sp": s, "tp": row_peer(db)}, device_id_type=MESH)
    pl.semaphore_wait(barrier, sp - 1 + A - 1 + B - 1)

    def send_w(da, k):
        rows = pl.ds(k * w_rows, w_rows)
        return pltpu.make_async_remote_copy(
            src_ref=w.at[0, core, rows], dst_ref=w.at[da, core, rows],
            send_sem=w_send.at[da - 1, k], recv_sem=w_recv.at[da - 1, k],
            device_id={"sp": s, "tp": column_peer(da)}, device_id_type=MESH,
        )

    def forward_w(da, k):
        rows = pl.ds(k * w_rows, w_rows)
        return pltpu.make_async_remote_copy(
            src_ref=w.at[da, core, rows], dst_ref=w.at[da, core, rows],
            send_sem=f_send.at[da - 1, k], recv_sem=f_recv.at[da - 1, k],
            device_id={"sp": partner, "tp": t}, device_id_type=MESH,
        )

    def arrived_w(da, k):
        rows = pl.ds(k * w_rows, w_rows)
        return pltpu.make_async_remote_copy(
            src_ref=w.at[da, 1 - core, rows], dst_ref=w.at[da, 1 - core, rows],
            send_sem=f_send.at[da - 1, k], recv_sem=f_recv.at[da - 1, k],
            device_id={"sp": partner, "tp": t}, device_id_type=MESH,
        )

    def send_x(db, i):
        return pltpu.make_async_remote_copy(
            src_ref=x.at[i], dst_ref=x.at[db * R + i],
            send_sem=x_send.at[(db - 1) * R + i], recv_sem=x_recv.at[(db - 1) * R + i],
            device_id={"sp": s, "tp": row_peer(db)}, device_id_type=MESH,
        )

    for k in range(2):
        local_w(k).wait()
    for k in range(W_CHUNKS):
        for da in range(1, A):
            send_w(da, k).start()
    for i in range(R):
        local_x(i).wait()
        for db in range(1, B):
            send_x(db, i).start()

    def normalise(r):
        for k in range(LANES // NORM_ROWS):
            here = pl.ds(k * NORM_ROWS, NORM_ROWS)
            flat = x[r, here, :].astype(jnp.float32)
            scale = lax.rsqrt(jnp.mean(flat * flat, axis=-1, keepdims=True) + epsilon)
            xn[r, here, :] = (flat * scale * gain[...]).astype(jnp.bfloat16)

    eye = lax.broadcasted_iota(jnp.int32, (HEAD, HEAD), 0) == lax.broadcasted_iota(jnp.int32, (HEAD, HEAD), 1)
    gain_column[...] = jnp.broadcast_to(
        jnp.sum(jnp.where(eye, key_gain[...], 0.0), axis=1, keepdims=True), (HEAD, LANES)
    )

    class Home:
        def __init__(self, r, da):
            db, i = r // R, r % R
            j, half = i // halves, i % halves
            rows_of = ((yb + B - db) % B) * A + (xa + da) % A
            seq = rows_of * seqs + j
            slot = r * A + da
            index = s * halves + half
            place = cache.at[:, :, pl.ds(pl.multiple_of(index * LANES, LANES), LANES)]
            block = out.at[r, 0] if isinstance(da, int) and da == 0 else relay.at[r, da - 1]
            self.here = seq == s
            self.remote = pltpu.make_async_remote_copy(
                src_ref=block, dst_ref=place, send_sem=o_send.at[slot], recv_sem=o_recv.at[index],
                device_id={"sp": seq, "tp": t}, device_id_type=MESH,
            )
            self.block, self.place, self.sem = block, place, o_recv.at[index]

        def start(self):
            @pl.when(self.here)
            def _():
                self.place[...] = self.block[...]

            @pl.when(jnp.logical_not(self.here))
            def _():
                self.remote.start()

        def wait_send(self):
            @pl.when(jnp.logical_not(self.here))
            def _():
                self.remote.wait_send()

    def hop(r, da):
        return pltpu.make_async_remote_copy(
            src_ref=out.at[r, da], dst_ref=relay.at[r, da - 1],
            send_sem=h_send.at[r, da - 1], recv_sem=h_recv.at[r, da - 1],
            device_id={"sp": s, "tp": yb * A + (xa + A - da) % A}, device_id_type=MESH,
        )

    def project(r, da):
        rows = xn[r]
        contract = (((1,), (1,)), ((), ()))
        raw = lax.dot_general(w[da, 0], rows, contract, preferred_element_type=jnp.float32)
        raw = raw.reshape(cols // HEAD, HEAD, LANES)
        scale = lax.rsqrt(jnp.mean(raw * raw, axis=1, keepdims=True) + epsilon)
        keys = raw * scale * gain_column[...][None]
        out[r, da, 0] = keys.reshape(cols, LANES).astype(jnp.bfloat16)
        out[r, da, 1] = lax.dot_general(
            w[da, 1], rows, contract, preferred_element_type=jnp.float32
        ).astype(jnp.bfloat16)

    def keep(r):
        project(r, 0)
        Home(r, 0).start()

    def give(r):
        def one(da, _):
            project(r, da)
            hop(r, da).start()
            return 0

        lax.fori_loop(1, A, one, 0)

    def pass_on(r):
        for da in range(1, A):
            hop(r, da).wait_recv()
            Home(r, da).start()

    def own_first(r, _):
        normalise(r)
        keep(r)
        return 0

    lax.fori_loop(0, R, own_first, 0)

    def take(n):
        i, db = n // (B - 1), 1 + n % (B - 1)
        send_x(db, i).wait_recv()
        r = db * R + i
        normalise(r)
        keep(r)
        return r

    N = R * (B - 1)
    theirs = [(1 + n % (B - 1)) * R + n // (B - 1) for n in range(N)]
    early = N // 2
    taken = 0
    for k in range(W_CHUNKS):
        for da in range(1, A):
            send_w(da, k).wait_recv()
            forward_w(da, k).start()
        while taken < early * (k + 1) // W_CHUNKS:
            take(taken)
            taken += 1
    for k in range(W_CHUNKS):
        for da in range(1, A):
            arrived_w(da, k).wait_recv()

    stays = (2 * t * seqs >= sp) == (2 * s >= sp)
    others_first = theirs[:early] + list(range(R))
    own_first_order = list(range(R)) + theirs[:early]
    order = [jnp.where(stays, a, b) for a, b in zip(others_first, own_first_order)]
    order += theirs[early:]
    given, passed = 0, 0
    for r in order[: early + R]:
        give(r)
        given += 1
        if given > early:
            pass_on(order[passed])
            passed += 1
    for n in range(early, N):
        give(take(n))
        given += 1
        while passed < (given if n == N - 1 else given - 1):
            pass_on(order[passed])
            passed += 1
    while passed < len(order):
        pass_on(order[passed])
        passed += 1

    for k in range(W_CHUNKS):
        for da in range(1, A):
            send_w(da, k).wait_send()
            forward_w(da, k).wait_send()
    for i in range(R):
        for db in range(1, B):
            send_x(db, i).wait_send()

    for r in range(B * R):
        for da in range(A):
            Home(r, da).wait_send()
            if da:
                hop(r, da).wait_send()

    def arrived(n):
        place = cache.at[:, :, pl.ds(pl.multiple_of(n * LANES, LANES), LANES)]
        pltpu.make_async_copy(out.at[0, 0], place, o_recv.at[n]).wait()

    def landed(n, _):
        @pl.when(n // halves != s)
        def _():
            arrived(n)

        return 0

    lax.fori_loop(0, sp * halves, landed, 0)


def read(dims, queries, bias, cache, keys_out, values_out, first_out, sems):
    group, heads, cols, length = dims
    rows = group * heads
    t = lax.axis_index("tp")
    keys, values = cache.at[0], cache.at[1]
    out_k = pltpu.make_async_copy(keys, keys_out.at[0], sems.at[2])
    out_v = pltpu.make_async_copy(values, values_out.at[0], sems.at[3])
    out_k.start()
    out_v.start()

    def spread(ref_value):
        n = ref_value.shape[1]
        parts = [jnp.broadcast_to(ref_value[g : g + 1], (heads, n)) for g in range(group)]
        return jnp.concatenate(parts, axis=0)

    row_head = lax.broadcasted_iota(jnp.int32, (rows, cols), 0) % heads
    own = (lax.broadcasted_iota(jnp.int32, (rows, cols), 1) // HEAD) == row_head
    query = jnp.where(own, spread(queries[...].astype(jnp.float32)), 0.0).astype(jnp.bfloat16)
    offsets = spread(bias[...])
    at = lax.broadcasted_iota(jnp.int32, offsets.shape, 1)
    mine = at == t * heads + lax.broadcasted_iota(jnp.int32, offsets.shape, 0) % heads
    offset = jnp.sum(jnp.where(mine, offsets, 0.0), axis=1, keepdims=True)

    scores = jnp.dot(query, keys[...], preferred_element_type=jnp.float32)
    scores = scores / math.sqrt(HEAD) + offset
    soft = jnp.log1p(jnp.exp(-jnp.abs(scores)))
    log_break = jnp.minimum(scores, 0.0) - soft
    log_keep = jnp.minimum(-scores, 0.0) - soft
    lane = lax.broadcasted_iota(jnp.int32, (rows, length), 1)

    def ahead(v, k):
        return jnp.where(lane < length - k, pltpu.roll(v, length - k, 1), 0.0)

    later = ahead(log_keep, 1)
    k = 1
    while k < length:
        if 4 * k <= length:
            later = (later + ahead(later, k)) + (ahead(later, 2 * k) + ahead(later, 3 * k))
            k *= 4
        else:
            later = later + ahead(later, k)
            k *= 2
    weights = jnp.exp(log_break + later).astype(jnp.bfloat16)
    taken = lax.dot_general(
        weights, values[...], (((1,), (1,)), ((), ())), preferred_element_type=jnp.float32
    )
    taken = jnp.where(own, taken, 0.0)
    for g in range(group):
        first_out[g : g + 1, :] = jnp.sum(
            taken[g * heads : (g + 1) * heads], axis=0, keepdims=True
        ).astype(jnp.bfloat16)
    out_k.wait()
    out_v.wait()


def local(prompt, input_gain, key_weight, value_weight, key_gain, queries, score_bias):
    sp, tp = lax.axis_size("sp"), lax.axis_size("tp")
    seq_here, pos_here, width = prompt.shape
    cols = key_weight.shape[0]
    group = queries.shape[1]
    A = 2 ** (int(math.log2(tp)) // 2)
    B = tp // A
    halves = pos_here // LANES
    R = seq_here * halves
    length = pos_here * sp
    hbm, vmem = pl.BlockSpec(memory_space=pl.ANY), pl.BlockSpec(memory_space=pltpu.VMEM)
    dma = pltpu.SemaphoreType.DMA
    bf16 = jnp.bfloat16
    cache = pl.pallas_call(
        functools.partial(produce, (sp, tp, A, B, R, halves, cols, width)),
        out_shape=pltpu.VMEM((2, cols, length), bf16),
        in_specs=[hbm, vmem, hbm, hbm, vmem],
        out_specs=vmem,
        scratch_shapes=[
            pltpu.VMEM((B * R, LANES, width), bf16),
            pltpu.VMEM((B * R, LANES, width), bf16),
            pltpu.VMEM((A, 2, cols, width), bf16),
            pltpu.VMEM((B * R, A, 2, cols, LANES), bf16),
            pltpu.VMEM((B * R, A - 1, 2, cols, LANES), bf16),
            pltpu.VMEM((HEAD, LANES), jnp.float32),
            dma((R,)),
            dma((2,)),
            dma(((B - 1) * R,)),
            dma(((B - 1) * R,)),
            dma((A - 1, W_CHUNKS)),
            dma((A - 1, W_CHUNKS)),
            dma((A - 1, W_CHUNKS)),
            dma((A - 1, W_CHUNKS)),
            dma((B * R, A - 1)),
            dma((B * R, A - 1)),
            dma((B * R * A,)),
            dma((sp * halves,)),
        ],
        compiler_params=pltpu.CompilerParams(
            collective_id=0, has_side_effects=True, vmem_limit_bytes=56 * 1024 * 1024
        ),
        name="produce",
    )(
        prompt.reshape(R, LANES, width),
        input_gain.reshape(1, width),
        key_weight,
        value_weight,
        key_gain.reshape(1, HEAD),
    )
    cache = pltpu.with_memory_space_constraint(cache, pltpu.VMEM)
    keys, values, first = pl.pallas_call(
        functools.partial(read, (group, cols // HEAD, cols, length)),
        out_shape=(
            jax.ShapeDtypeStruct((1, cols, length), bf16),
            jax.ShapeDtypeStruct((1, cols, length), bf16),
            jax.ShapeDtypeStruct((group, cols), bf16),
        ),
        in_specs=[vmem, vmem, vmem],
        out_specs=(hbm, hbm, vmem),
        scratch_shapes=[dma((4,))],
        name="read",
    )(queries.reshape(group, cols), score_bias, cache)
    return keys, values, first.reshape(1, group, cols)


def solution(mesh):
    placed = (P("tp", "sp", None), P(), P("tp", None), P("tp", None), P(), P("sp", None, "tp"), P())
    return jax.shard_map(
        local,
        mesh=mesh,
        in_specs=placed,
        out_specs=(P("sp", "tp", None), P("sp", "tp", None), P("sp", None, "tp")),
        check_vma=False,
    )
```
